512 devices in a mesh: sp: 64 (over z, y), tp: 8 (over x, core).
Axes of the slice: x: 4, y: 8, z: 8, core: 2. Of those that a mesh axis runs over, the one named last changes fastest.
Arguments:
- tokens: bfloat16 [32768, 2048], P('sp', 'tp'), may hold values from -6 to 6
- input_gain: bfloat16 [2048], P('tp'), may hold values from 0.099609375 to 1.8984375
- query_weight: bfloat16 [2048, 1024], P(None, 'tp'), may hold values from -10 to 10
- key_weight: bfloat16 [2048, 1024], P(None, 'tp'), may hold values from -10 to 10
- value_weight: bfloat16 [2048, 1024], P(None, 'tp'), may hold values from -0.125 to 0.125
- pool_in_weight: bfloat16 [2048, 1024], P(None, 'tp'), may hold values from -0.125 to 0.125
- log_gates: float32 [8, 32768], P('tp'), may hold values from -32768 to 0, as said below
- pool_weight: bfloat16 [8, 128, 128], P('tp'), may hold values from -0.5 to 0.5
- pool_scale: float32 [1024], P('tp'), may hold values from 0.1 to 1.9
- attention_out: bfloat16 [1024, 2048], P('tp'), may hold values from -16 to 16
- pooling_out: bfloat16 [1024, 2048], P('tp'), may hold values from -16 to 16
- final_gain: float32 [2048], P('tp'), may hold values from 0.1 to 1.9
Outputs:
- layer_out: bfloat16 [32768, 2048], P('sp', 'tp')
The draws below stay inside these ranges and needn't reach their ends.
Inputs may be any that keep to these rules, and one draw needn't show every extreme that they name: `log_gates`: each row does not increase along positions.
All inputs are finite; a program needn't handle non-finite values.
Results may differ from the reference program's by a relative error of at most 0.015.
Values may be sent and summed in bfloat16 or wider, within the bound.
No kernel may reach another device: no remote copies, remote signals or barrier semaphores. Data moves between devices by JAX's collectives and lax.ppermute only.
A program may use at most 128 MiB of HBM per device.

```python
import math
import jax
import jax.numpy as jnp
from jax import lax

D = 2048
HEAD = 128
ATT_HEADS = 8
POOL_GROUPS = 8
TOK_DEV = 512
TOKENS = 32768


def pair_bases(key):
    first = jnp.clip(jax.random.normal(jax.random.fold_in(key, 101), (D, ATT_HEADS * HEAD), jnp.float32), -4.0, 4.0)
    second = jnp.clip(jax.random.normal(jax.random.fold_in(key, 102), (D, ATT_HEADS * HEAD), jnp.float32), -4.0, 4.0)
    return (first, second)


def draw_query_weight(key, part):
    first, second = pair_bases(key)
    drawn = first
    return (drawn * D ** (-0.5)).astype(jnp.bfloat16)


def draw_key_weight(key, part):
    first, second = pair_bases(key)
    drawn = 3.0 * second
    return (drawn * D ** (-0.5)).astype(jnp.bfloat16)


def draw_log_gates(key, part):
    heads = ATT_HEADS
    order = jax.random.permutation(jax.random.fold_in(key, 31), heads)
    slow = order < heads // 2
    forget_span = jnp.exp(jax.random.uniform(jax.random.fold_in(key, 32), (heads,), jnp.float32, math.log(30.0), math.log(100.0)))
    starting_shift_amount = jnp.where(slow, 0.55 / TOKENS, 1.0 / forget_span)
    approximate_guess = jnp.exp(jax.random.uniform(jax.random.fold_in(key, 33), (heads, TOKENS), jnp.float32, -math.log(4.0), math.log(4.0)))
    blocks = jnp.exp(jax.random.uniform(jax.random.fold_in(key, 34), (heads, TOKENS // TOK_DEV), jnp.float32, -math.log(2.0), math.log(2.0)))
    tile_scaling_factor = jnp.repeat(blocks, TOK_DEV, axis=1)
    seat_indices = jax.random.randint(jax.random.fold_in(key, 35), (heads, 2), 0, TOKENS)
    objective_numbers = jnp.log(jax.random.uniform(jax.random.fold_in(key, 36), (heads, 2), jnp.float32, 0.5, 0.8))
    element_locations = jnp.arange(TOKENS, dtype=jnp.int32)
    segment_clusters = jnp.sum(jnp.where(element_locations[None, None, :] == seat_indices[:, :, None], objective_numbers[:, :, None], 0.0), axis=1)
    return jnp.cumsum(segment_clusters - starting_shift_amount[:, None] * approximate_guess * tile_scaling_factor, axis=1).astype(jnp.float32)


def rising_weight(key, rows, salt):
    noise = jnp.clip(jax.random.normal(jax.random.fold_in(key, salt), (rows, D), jnp.float32), -4.0, 4.0)
    highest = 10.0
    jitter = jnp.exp(jax.random.uniform(jax.random.fold_in(key, salt + 1), (D,), jnp.float32, -0.35, 0.35))
    rising = jnp.exp(math.log(highest) * jnp.arange(D, dtype=jnp.float32) / D) * jitter
    return (noise * rising[None, :] * rows ** (-0.5)).astype(jnp.bfloat16)


def draw_attention_out(key, part):
    return rising_weight(key, ATT_HEADS * HEAD, 41)


def draw_pooling_out(key, part):
    return rising_weight(key, POOL_GROUPS * HEAD, 51)


def levels(rng, dims, shards, low, largest):
    def one(dim, blocks):
        heights = jax.random.uniform(jax.random.fold_in(jax.random.fold_in(rng, 6), dim), (blocks,), jnp.float32, low / len(shards), largest / len(shards))
        return jnp.repeat(jnp.exp(heights), dims[dim] // blocks).reshape((-1,) + (1,) * (len(dims) - dim - 1))

    gain = one(*shards[0])
    for cut in shards[1:]:
        gain = gain * one(*cut)
    return gain


def bell_draw(stream_key, shape, scale, bound, split=(), kind=jnp.bfloat16):
    level = levels(stream_key, shape, split, -0.22, 0.18) if split else 1.0
    values = jax.random.normal(stream_key, shape, jnp.float32) * scale * level
    return jnp.minimum(jnp.maximum(values, -bound), bound).astype(kind)


def setup_inputs(seed: int = 0) -> dict:
    splits = jax.random.split(jax.random.key(seed), 13)
    tokens = bell_draw(splits[0], (TOKENS, D), 1.0, 6.0, ((0, 64), (1, 8)))
    input_gain = jnp.clip(1.0 + 0.18 * jax.random.normal(splits[1], (D,), jnp.float32), 0.099609375, 1.8984375).astype(jnp.bfloat16)
    query_weight = draw_query_weight(jax.random.fold_in(splits[12], 71), 0)
    key_weight = draw_key_weight(jax.random.fold_in(splits[12], 71), 0)
    value_weight = bell_draw(splits[4], (D, ATT_HEADS * HEAD), D ** -0.5, 0.125, ((1, 8),))
    pool_in_weight = bell_draw(splits[5], (D, POOL_GROUPS * HEAD), D ** -0.5, 0.125, ((1, 8),))
    log_gates = draw_log_gates(jax.random.fold_in(splits[12], 71), 0)
    pool_weight = bell_draw(splits[7], (POOL_GROUPS, HEAD, HEAD), HEAD ** -0.5, 0.5, ((0, 8),))
    pool_scale = jnp.clip(1.0 + 0.18 * jax.random.normal(splits[8], (POOL_GROUPS * HEAD,), jnp.float32), 0.1, 1.9)
    attention_out = draw_attention_out(jax.random.fold_in(splits[12], 71), 0)
    pooling_out = draw_pooling_out(jax.random.fold_in(splits[12], 71), 0)
    final_gain = jnp.clip(1.0 + 0.18 * jax.random.normal(splits[11], (D,), jnp.float32), 0.1, 1.9)
    return {"tokens": tokens, "input_gain": input_gain, "query_weight": query_weight, "key_weight": key_weight, "value_weight": value_weight, "pool_in_weight": pool_in_weight, "log_gates": log_gates, "pool_weight": pool_weight, "pool_scale": pool_scale, "attention_out": attention_out, "pooling_out": pooling_out, "final_gain": final_gain}


epsilon = 1e-06

def attention(query, keys, values, log_gates):
    total_rows = query.shape[0]
    heads = log_gates.shape[0]
    head_size = query.shape[1] // heads
    block = math.gcd(total_rows, 256)
    query_blocks = query.reshape(total_rows // block, block, heads, head_size).astype(jnp.float32)
    keys_whole = keys.reshape(total_rows, heads, head_size).astype(jnp.float32)
    values_whole = values.reshape(total_rows, heads, head_size).astype(jnp.float32)
    key_rows = jnp.arange(total_rows, dtype=jnp.int32)

    def one_block(args):
        query_block, first = args
        query_gate = lax.dynamic_slice_in_dim(log_gates, first, block, 1).T
        scores = jnp.einsum('thd,shd->ths', query_block, keys_whole) * head_size ** (-0.5)
        scores = scores + query_gate[:, :, None] - log_gates[None, :, :]
        rows = first + jnp.arange(block, dtype=jnp.int32)
        allowed = (rows[:, None] >= key_rows[None, :])[:, None, :]
        scores = jnp.where(allowed, scores, -jnp.inf)
        row_max = lax.optimization_barrier(jnp.max(scores, axis=2, keepdims=True))
        weights = jnp.exp(scores - row_max)
        totals = lax.optimization_barrier(jnp.sum(weights, axis=2))
        rounded = lax.optimization_barrier(weights.astype(jnp.bfloat16)).astype(jnp.float32)
        result = jnp.einsum('ths,shd->thd', rounded, values_whole) / totals[:, :, None]
        return result.astype(jnp.bfloat16)
    block_starts = jnp.arange(total_rows // block, dtype=jnp.int32) * block
    result = lax.map(one_block, (query_blocks, block_starts))
    return result.reshape(total_rows, heads * head_size)

def pooling(pool_input, pool_weight, pool_scale):
    total_rows, width = pool_input.shape
    groups = pool_weight.shape[0]
    head_size = pool_weight.shape[1]
    widened = pool_input.astype(jnp.float32)
    running = jnp.cumsum(widened, axis=0)
    padded = jnp.concatenate([jnp.zeros((1, width), jnp.float32), running], axis=0)
    rows = jnp.arange(total_rows, dtype=jnp.int32)[:, None]
    column = jnp.arange(width, dtype=jnp.int32)
    window = jnp.left_shift(jnp.full((width,), 2, jnp.int32), column // head_size % 4)
    lower = jnp.maximum(rows + 1 - window[None, :], 0).astype(jnp.int32)
    counts = (rows + 1 - lower).astype(jnp.float32)
    window_sum = running - jnp.take_along_axis(padded, lower, axis=0)
    departure = (window_sum / counts - widened).astype(jnp.bfloat16)
    mapped = jnp.einsum('tgc,gcd->tgd', departure.reshape(total_rows, groups, head_size).astype(jnp.float32), pool_weight.astype(jnp.float32))
    return (mapped.reshape(total_rows, width) * pool_scale).astype(jnp.bfloat16)

def reference(tokens, input_gain, query_weight, key_weight, value_weight, pool_in_weight, log_gates, pool_weight, pool_scale, attention_out, pooling_out, final_gain):
    widened = tokens.astype(jnp.float32)
    inverse = lax.rsqrt(lax.optimization_barrier(jnp.mean(widened * widened, axis=1)) + epsilon)[:, None]
    scaled = (widened * input_gain.astype(jnp.float32)).astype(jnp.bfloat16)

    def project(weight):
        return (jnp.dot(scaled, weight, preferred_element_type=jnp.float32) * inverse).astype(jnp.bfloat16)
    attended = attention(project(query_weight), project(key_weight), project(value_weight), log_gates)
    pooled = pooling(project(pool_in_weight), pool_weight, pool_scale)
    mixed = jnp.dot(attended, attention_out, preferred_element_type=jnp.float32) + jnp.dot(pooled, pooling_out, preferred_element_type=jnp.float32)
    out_inverse = lax.rsqrt(lax.optimization_barrier(jnp.mean(mixed * mixed, axis=1)) + epsilon)[:, None]
    return (mixed * out_inverse * final_gain).astype(jnp.bfloat16)
```

```python
import functools
import math

import numpy as np
import jax
import jax.numpy as jnp
from jax import lax
from jax.experimental import pallas as pl
from jax.experimental.pallas import tpu as pltpu
from jax.sharding import PartitionSpec as P

BF = jnp.bfloat16
F32 = jnp.float32
LOW = -1e30
EPS = 1e-06
LOG2E = math.log2(math.e)
RIM = 16
BOTH = ("sp", "tp")
SIDE = 8

VM = pl.BlockSpec(memory_space=pltpu.VMEM)
SM = pl.BlockSpec(memory_space=pltpu.SMEM)
ROOM = pltpu.CompilerParams(vmem_limit_bytes=56 * 2**20)


def scratch(shape, dtype):
    return pltpu.VMEM(shape, dtype)


def ring(z, y, p, along_y):
    return [((z * SIDE + i) if along_y else (i * SIDE + y)) * 8 + p for i in range(SIDE)]


def rings(for_keys):
    groups = []
    for p in range(8):
        along_y = (p % 2 == 0) == for_keys
        for i in range(SIDE):
            groups.append(ring(i, i, p, along_y))
    return groups


def work_table():
    steps = SIDE * SIDE + 4
    table = np.zeros((2, SIDE, SIDE, 2 * steps + 8), np.int32)
    for odd in range(2):
        for z in range(SIDE):
            for y in range(SIDE):
                row = table[odd, z, y]
                mine = np.arange(SIDE)
                if odd:
                    q_blocks, k_blocks = z * SIDE + mine, mine * SIDE + y
                else:
                    q_blocks, k_blocks = mine * SIDE + y, z * SIDE + mine
                pairs = [(i, j) for i in range(SIDE) for j in range(SIDE) if q_blocks[i] > k_blocks[j]]
                cross = [(i, j) for i in range(SIDE) for j in range(SIDE) if q_blocks[i] == k_blocks[j]]
                (dq, dk), = cross
                for t in range(steps):
                    i, j = pairs[min(t, len(pairs) - 1)] if pairs else (dq, dk)
                    row[t], row[steps + t] = i, j
                needed = 1 + max([dk] + [j for _, j in pairs])
                row[2 * steps :] = [
                    len(pairs), needed, dq, dk,
                    q_blocks[0], q_blocks[1] - q_blocks[0], k_blocks[0], k_blocks[1] - k_blocks[0],
                ]
    return table.reshape(2, SIDE * SIDE, -1)


def split3(x):
    high = x.astype(BF).astype(F32)
    rest = x - high
    mid = rest.astype(BF).astype(F32)
    return high, mid, rest - mid


def dot(a, b, ca=1, cb=0):
    return lax.dot_general(a, b, (((ca,), (cb,)), ((), ())), preferred_element_type=F32)


def project_kernel(where, own, other, wq, wk, wv, wp, q_out, kv_out, p_out, *, rows, factor):
    odd = where[0]
    wide = own.shape[2]
    squares = jnp.zeros((rows, wide), F32)
    qp = jnp.zeros((rows, 2 * 128), F32)
    kv = jnp.zeros((rows, 2 * 128), F32)
    for ref, parity in ((own, odd), (other, 1 - odd)):
        for x in range(own.shape[0]):
            at = pl.multiple_of((2 * x + parity) * wide, wide)
            t = ref[x, :rows, :].astype(F32)
            gain = ref[x, rows : rows + 1, :].astype(F32)
            squares = squares + t * t
            s = (t * gain).astype(BF)
            w1 = jnp.concatenate([wq[pl.ds(at, wide), :], wp[pl.ds(at, wide), :]], axis=1)
            w2 = jnp.concatenate([wk[pl.ds(at, wide), :], wv[pl.ds(at, wide), :]], axis=1)
            qp = qp + dot(s, w1)
            kv = kv + dot(s, w2)
    width = wq.shape[0]
    inverse = lax.rsqrt(jnp.sum(squares, axis=1, keepdims=True) / width + EPS)
    q = (qp[:, :128] * (inverse * factor)).astype(BF)
    p_out[...] = (qp[:, 128:] * inverse).astype(BF)
    kv = (kv * inverse).astype(BF)
    for i in range(SIDE):
        q_out[i] = q
        kv_out[i] = kv


def project(where, own, other, wq, wk, wv, wp, rows, head):
    factor = head ** (-0.5) * LOG2E
    return pl.pallas_call(
        functools.partial(project_kernel, rows=rows, factor=factor),
        out_shape=(
            jax.ShapeDtypeStruct((SIDE, rows, head), BF),
            jax.ShapeDtypeStruct((SIDE, rows, 2 * head), BF),
            jax.ShapeDtypeStruct((rows, head), BF),
        ),
        in_specs=[SM] + [VM] * 6,
        out_specs=(VM, VM, VM),
        compiler_params=ROOM,
        name="project",
    )(where, own, other, wq, wk, wv, wp)


def attend_kernel(tab, base, q_ref, kv_ref, gates, o_ref, kaug, qaug, vt, acc, tops, sa, sb, ma, mb):
    count, blk, hd = q_ref.shape
    aug = vt.shape[1]
    steps = (tab.shape[0] - 8) // 2
    n, needed, dq, dk, q0, qs, k0, ks = [tab[2 * steps + i] for i in range(8)]
    col = lax.broadcasted_iota(jnp.int32, (blk, hd), 1)
    ones = jnp.where(col < 3, 1.0, 0.0).astype(BF)
    row = lax.broadcasted_iota(jnp.int32, (hd, blk), 0)
    tail = lax.broadcasted_iota(jnp.int32, (aug - hd, blk), 0)
    count_row = jnp.where(tail == 0, 1.0, 0.0).astype(BF)

    def prepare_keys(j, c):
        g = gates[pl.ds(k0 + j * ks, 1), :]
        high, mid, low = split3((g[:, :1] - g) * LOG2E)
        b = jnp.where(row == 0, high, jnp.where(row == 1, mid, jnp.where(row == 2, low, 0.0)))
        kaug[j, :, :hd] = kv_ref[j, :, :hd]
        kaug[j, :, hd:] = b.T.astype(BF)
        vt[j, :hd, :] = kv_ref[j, :, hd:].T
        vt[j, hd:, :] = count_row
        return c

    lax.fori_loop(0, needed, prepare_keys, 0)

    def prepare_queries(j, c):
        qaug[j, :, :hd] = q_ref[j]
        qaug[j, :, hd:] = ones
        tops[j] = jnp.full((1, blk), LOW, F32)
        acc[j] = jnp.zeros((aug, blk), F32)
        return c

    lax.fori_loop(0, count, prepare_queries, 0)

    def shift(qi, ki):
        return (base[q0 + qi * qs] - base[k0 + ki * ks]) * LOG2E

    def scores(qi, ki):
        return dot(kaug[ki], qaug[qi], 1, 1)

    def start(t, s_ref, m_ref):
        s = scores(tab[t], tab[steps + t])
        s_ref[...] = s
        m_ref[...] = jnp.max(s, axis=0, keepdims=True)

    def finish(t, s_ref, m_ref):
        qi, ki = tab[t], tab[steps + t]
        sh = jnp.where(t < n, shift(qi, ki), LOW)
        before = tops[qi]
        after = jnp.maximum(before, m_ref[...] + sh)
        tops[qi] = after
        weight = jnp.exp2(s_ref[...] - (after - sh)).astype(BF)
        acc[qi] = acc[qi] * jnp.exp2(before - after) + dot(vt[ki], weight)

    key = lax.broadcasted_iota(jnp.int32, (blk, blk), 0)
    query = lax.broadcasted_iota(jnp.int32, (blk, blk), 1)
    s = jnp.where(key <= query, scores(dq, dk), LOW)
    top = jnp.max(s, axis=0, keepdims=True)
    tops[dq] = top
    acc[dq] = dot(vt[dk], jnp.exp2(s - top).astype(BF))

    start(0, sa, ma)

    def two_steps(i, c):
        t = 2 * i
        start(t + 1, sb, mb)
        finish(t, sa, ma)
        start(t + 2, sa, ma)
        finish(t + 1, sb, mb)
        return c

    lax.fori_loop(0, (n + 1) // 2, two_steps, 0)

    def close(j, c):
        total = acc[j, hd : hd + 1, :]
        some = total > 0.0
        safe = jnp.where(some, total, 1.0)
        over = jnp.where(some, 1.0 / safe, 0.0)
        high, mid, low = split3(jnp.where(some, tops[j] + jnp.log2(safe), LOW))
        o_ref[j, :hd, :] = (acc[j, :hd, :] * over).astype(BF)
        o_ref[j, hd:, :] = jnp.where(
            tail == 0, high, jnp.where(tail == 1, mid, jnp.where(tail == 2, low, 0.0))
        ).astype(BF)
        return c

    lax.fori_loop(0, count, close, 0)


def attend(tab, base, q, kv, gates):
    count, blk, hd = q.shape
    aug = hd + 16
    return pl.pallas_call(
        attend_kernel,
        out_shape=jax.ShapeDtypeStruct((count, aug, blk), BF),
        in_specs=[SM, SM, VM, VM, VM],
        out_specs=VM,
        scratch_shapes=[
            scratch((count, blk, 2 * hd), BF),
            scratch((count, blk, 2 * hd), BF),
            scratch((count, aug, blk), BF),
            scratch((count, aug, blk), F32),
            scratch((count, 1, blk), F32),
            scratch((blk, blk), F32),
            scratch((blk, blk), F32),
            scratch((1, blk), F32),
            scratch((1, blk), F32),
        ],
        compiler_params=ROOM,
        name="attend",
    )(tab, base, q, kv, gates)


def mix_kernel(where, parts, pool_in, rim, pool_weight, pool_scale, ap_out, wide):
    hd = pool_weight.shape[0]
    rows = pool_in.shape[0]
    count = parts.shape[0]
    lse = []
    for j in range(count):
        t = parts[j, hd : hd + 16, :].astype(F32)
        lse.append(t[0:1] + t[1:2] + t[2:3])
    top = functools.reduce(jnp.maximum, lse)
    total = jnp.zeros_like(top)
    summed = jnp.zeros((hd, rows), F32)
    for j in range(count):
        w = jnp.exp2(lse[j] - top)
        total = total + w
        summed = summed + parts[j, :hd, :].astype(F32) * w
    ap_out[:, :hd] = (summed / total).T.astype(BF)

    first, window = where[1], where[2]
    here = pool_in[...].astype(F32)
    edge = jnp.where(first > 0, rim[...].astype(F32), 0.0)
    wide[:RIM, :] = edge
    wide[RIM:, :] = here
    sums = wide[...]
    span = 1
    chosen = jnp.zeros((rows, hd), F32)
    while span < RIM:
        length = sums.shape[0] - span
        sums = sums[span:, :] + sums[:length, :]
        span *= 2
        at = RIM - span + 1
        chosen = jnp.where(window == span, sums[at : at + rows, :], chosen)
    place = first + lax.broadcasted_iota(jnp.int32, (rows, hd), 0)
    counts = jnp.minimum(window, place + 1).astype(F32)
    departure = (chosen / counts - here).astype(BF)
    ap_out[:, hd:] = (dot(departure, pool_weight[...]) * pool_scale[...]).astype(BF)


def mix(where, parts, pool_in, rim, pool_weight, pool_scale):
    rows, hd = pool_in.shape
    return pl.pallas_call(
        mix_kernel,
        out_shape=jax.ShapeDtypeStruct((rows, 2 * hd), BF),
        in_specs=[SM] + [VM] * 5,
        out_specs=VM,
        scratch_shapes=[scratch((rows + RIM, hd), F32)],
        compiler_params=ROOM,
        name="mix",
    )(where, parts, pool_in, rim, pool_weight, pool_scale)


def out_kernel(where, mine, theirs, wa, wp, wt, out):
    odd = where[0]
    rows = mine.shape[0]
    hd = wa.shape[0]
    a = jnp.concatenate([mine[...], theirs[...]], axis=1)
    for x in range(out.shape[0]):
        wide = out.shape[2]
        at = pl.multiple_of((2 * x + odd) * wide, wide)
        w = jnp.concatenate(
            [wa[:, pl.ds(at, wide)], wp[:, pl.ds(at, wide)], wt[:, x * wide : (x + 1) * wide]], axis=0
        )
        out[x] = dot(a, w).astype(BF)


def out_project(where, mine, theirs, wa, wp, wt, chips):
    rows = mine.shape[0]
    wide = wt.shape[1] // chips
    return pl.pallas_call(
        out_kernel,
        out_shape=jax.ShapeDtypeStruct((chips, rows, wide), BF),
        in_specs=[SM] + [VM] * 5,
        out_specs=VM,
        compiler_params=ROOM,
        name="out_project",
    )(where, mine, theirs, wa, wp, wt)


def square_kernel(parts, mixed_out, sq_out):
    rows, wide = mixed_out.shape
    mixed = functools.reduce(lambda a, b: a + b, [parts[x].astype(F32) for x in range(parts.shape[0])])
    mixed_out[...] = mixed
    sq = mixed * mixed
    lanes = functools.reduce(lambda a, b: a + b, [sq[:, i : i + 128] for i in range(0, wide, 128)])
    for r in range(rows // 128):
        line = jnp.sum(lanes[r * 128 : (r + 1) * 128, :].T, axis=0, keepdims=True)
        for i in range(sq_out.shape[0]):
            sq_out[i, r : r + 1, :] = line


def square(parts):
    chips, rows, wide = parts.shape
    return pl.pallas_call(
        square_kernel,
        out_shape=(
            jax.ShapeDtypeStruct((rows, wide), F32),
            jax.ShapeDtypeStruct((8, rows // 128, 128), F32),
        ),
        in_specs=[VM],
        out_specs=(VM, VM),
        compiler_params=ROOM,
        name="square",
    )(parts)


def finish_kernel(mixed, sq, gain, out, *, width):
    total = functools.reduce(lambda a, b: a + b, [sq[i] for i in range(sq.shape[0])])
    inverse = lax.rsqrt(total / width + EPS)
    for r in range(total.shape[0]):
        each = jnp.broadcast_to(inverse[r : r + 1, :], (128, 128)).T
        for c in range(0, mixed.shape[1], 128):
            at = slice(r * 128, (r + 1) * 128)
            out[at, c : c + 128] = (mixed[at, c : c + 128] * each * gain[:, c : c + 128]).astype(BF)


def finish_rows(mixed, sq, gain, width):
    rows, wide = mixed.shape
    return pl.pallas_call(
        functools.partial(finish_kernel, width=width),
        out_shape=jax.ShapeDtypeStruct((rows, wide), BF),
        in_specs=[VM] * 3,
        out_specs=VM,
        compiler_params=ROOM,
        name="finish",
    )(mixed, sq, gain)


CHIPS = [[0, 2, 4, 6], [1, 3, 5, 7]]
PARTNER = [(i, i ^ 1) for i in range(8)]


def exchange(blocks, axis, groups):
    return lax.all_to_all(blocks, axis, 0, 0, axis_index_groups=groups, tiled=True)


def body(
    tokens,
    input_gain,
    query_weight,
    key_weight,
    value_weight,
    pool_in_weight,
    log_gates,
    pool_weight,
    pool_scale,
    attention_out,
    pooling_out,
    final_gain,
):
    rows, wide = tokens.shape
    width = query_weight.shape[0]
    hd = pool_weight.shape[1]
    sp = lax.axis_index("sp")
    tp = lax.axis_index("tp")
    odd = tp % 2
    where = jnp.stack([odd, sp * rows, jnp.left_shift(2, tp % 4)]).astype(jnp.int32)

    def for_partner(w):
        return lax.dynamic_index_in_dim(w.reshape(hd, 4, 2, wide), 1 - odd, 2, keepdims=False).reshape(hd, 4 * wide)

    theirs = jnp.concatenate([for_partner(attention_out), for_partner(pooling_out)], axis=0)
    partner_weight = lax.ppermute(theirs, "tp", PARTNER)

    extended = jnp.concatenate([tokens, jnp.broadcast_to(input_gain, (16, wide))], axis=0)
    own = exchange(jnp.broadcast_to(extended, (4, rows + 16, wide)), "tp", CHIPS)
    other = lax.ppermute(own, "tp", PARTNER)
    q, kv, pool_in = project(
        where, own, other, query_weight, key_weight, value_weight, pool_in_weight, rows, hd
    )

    sequence = lax.axis_size("sp")
    rim = lax.ppermute(pool_in[rows - RIM :], "sp", [(i, i + 1) for i in range(sequence - 1)])
    q = exchange(q, BOTH, rings(False))
    kv = exchange(kv, BOTH, rings(True))

    gates = log_gates.reshape(sequence, rows)
    table = jnp.asarray(work_table())
    tab = lax.dynamic_slice(table, (odd, sp, 0), (1, 1, table.shape[2])).reshape(-1)
    parts = attend(tab, gates[:, 0], q, kv, gates)
    parts = exchange(parts, BOTH, rings(False))

    ap = mix(where, parts, pool_in, rim, pool_weight[0], pool_scale.reshape(1, -1))
    ap_other = lax.ppermute(ap, "tp", PARTNER)
    shares = out_project(where, ap, ap_other, attention_out, pooling_out, partner_weight, 4)
    mixed, sq = square(exchange(shares, "tp", CHIPS))
    sq = lax.all_to_all(sq, "tp", 0, 0, tiled=True)
    return finish_rows(mixed, sq, final_gain.reshape(1, -1), width)


def solution(mesh):
    return jax.shard_map(
        body,
        mesh=mesh,
        in_specs=(
            P("sp", "tp"),
            P("tp"),
            P(None, "tp"),
            P(None, "tp"),
            P(None, "tp"),
            P(None, "tp"),
            P("tp", None),
            P("tp", None, None),
            P("tp"),
            P("tp", None),
            P("tp", None),
            P("tp"),
        ),
        out_specs=P("sp", "tp"),
        check_vma=False,
    )
```

```python
import functools
import math

import numpy as np
import jax
import jax.numpy as jnp
from jax import lax
from jax.experimental import pallas as pl
from jax.experimental.pallas import tpu as pltpu
from jax.sharding import PartitionSpec as P

BF = jnp.bfloat16
F32 = jnp.float32
LOW = -1e30
EPS = 1e-06
LOG2E = math.log2(math.e)
RIM = 16
BOTH = ("sp", "tp")
SIDE = 8
UNROLL = 4

VM = pl.BlockSpec(memory_space=pltpu.VMEM)
SM = pl.BlockSpec(memory_space=pltpu.SMEM)
ROOM = pltpu.CompilerParams(vmem_limit_bytes=56 * 2**20)


def scratch(shape, dtype):
    return pltpu.VMEM(shape, dtype)


def placed(shape, dtype):
    return pltpu.VMEM(shape, dtype)


def near(x):
    return pltpu.with_memory_space_constraint(x, pltpu.VMEM)


def ring(z, y, p, along_y):
    return [((z * SIDE + i) if along_y else (i * SIDE + y)) * 8 + p for i in range(SIDE)]


def rings(for_keys):
    groups = []
    for p in range(8):
        along_y = (p % 2 == 0) == for_keys
        for i in range(SIDE):
            groups.append(ring(i, i, p, along_y))
    return groups


def moved(distance):
    return [
        (group[i], group[(i + distance) % SIDE]) for group in rings(False) for i in range(SIDE)
    ]


def work_table():
    steps = SIDE * SIDE + UNROLL
    table = np.zeros((2, SIDE, SIDE, 2 * steps + 17), np.int32)
    for odd in range(2):
        for z in range(SIDE):
            for y in range(SIDE):
                row = table[odd, z, y]
                mine = np.arange(SIDE)
                if odd:
                    q_blocks, k_blocks = z * SIDE + mine, mine * SIDE + y
                else:
                    q_blocks, k_blocks = mine * SIDE + y, z * SIDE + mine
                pairs = [(i, j) for i in range(SIDE) for j in range(SIDE) if q_blocks[i] > k_blocks[j]]
                cross = [(i, j) for i in range(SIDE) for j in range(SIDE) if q_blocks[i] == k_blocks[j]]
                (dq, dk), = cross
                for t in range(steps):
                    i, j = pairs[min(t, len(pairs) - 1)] if pairs else (dq, dk)
                    row[t], row[steps + t] = i, j
                nearest = [max([j for i, j in pairs if i == own], default=0) for own in range(SIDE)]
                row[2 * steps :] = [
                    len(pairs), dq, dk,
                    q_blocks[0], q_blocks[1] - q_blocks[0], k_blocks[0], k_blocks[1] - k_blocks[0],
                    y if odd else z, *nearest, 0,
                ]
    return table.reshape(2, SIDE * SIDE, -1)


def split3(x):
    high = x.astype(BF).astype(F32)
    rest = x - high
    mid = rest.astype(BF).astype(F32)
    return high, mid, rest - mid


def dot(a, b, ca=1, cb=0):
    return lax.dot_general(a, b, (((ca,), (cb,)), ((), ())), preferred_element_type=F32)


def project_kernel(where, own, other, wq, wk, wv, wp, q_out, kv_out, p_out, *, rows, factor):
    odd = where[0]
    wide = own.shape[2]
    squares = jnp.zeros((rows, wide), F32)
    qp = jnp.zeros((rows, 2 * 128), F32)
    kv = jnp.zeros((rows, 2 * 128), F32)
    for ref, parity in ((own, odd), (other, 1 - odd)):
        for x in range(own.shape[0]):
            at = pl.multiple_of((2 * x + parity) * wide, wide)
            t = ref[x, :rows, :].astype(F32)
            gain = ref[x, rows : rows + 1, :].astype(F32)
            squares = squares + t * t
            s = (t * gain).astype(BF)
            w1 = jnp.concatenate([wq[pl.ds(at, wide), :], wp[pl.ds(at, wide), :]], axis=1)
            w2 = jnp.concatenate([wk[pl.ds(at, wide), :], wv[pl.ds(at, wide), :]], axis=1)
            qp = qp + dot(s, w1)
            kv = kv + dot(s, w2)
    width = wq.shape[0]
    inverse = lax.rsqrt(jnp.sum(squares, axis=1, keepdims=True) / width + EPS)
    q = (qp[:, :128] * (inverse * factor)).astype(BF)
    p_out[...] = (qp[:, 128:] * inverse).astype(BF)
    k = (kv[:, :128] * inverse).astype(BF)
    vt = (kv[:, 128:] * inverse).T.astype(BF)
    q_out[...] = q
    for i in range(SIDE):
        kv_out[i, :, :128] = k
        for r in range(0, rows, 128):
            kv_out[i, r : r + 128, 128:] = vt[:, r : r + 128]


def project(where, own, other, wq, wk, wv, wp, rows, head):
    factor = head ** (-0.5) * LOG2E
    return pl.pallas_call(
        functools.partial(project_kernel, rows=rows, factor=factor),
        out_shape=(
            placed((rows, head), BF),
            jax.ShapeDtypeStruct((SIDE, rows, 2 * head), BF),
            placed((rows, head), BF),
        ),
        in_specs=[SM] + [VM] * 6,
        out_specs=(VM, VM, VM),
        compiler_params=ROOM,
        name="project",
    )(where, own, other, wq, wk, wv, wp)


def attend_kernel(tab, base, *refs):
    arrivals, (kv_ref, gates, o_ref, qs, bias, acc, tops, pa, pb, sa) = refs[:SIDE], refs[SIDE:]
    count = SIDE
    blk, hd = arrivals[0].shape
    aug = acc.shape[1]
    steps = (tab.shape[0] - 17) // 2
    n, dq, dk, q0, qstep, k0, kstep, me = [tab[2 * steps + i] for i in range(8)]
    tail = lax.broadcasted_iota(jnp.int32, (aug - hd, blk), 0)
    count_row = jnp.where(tail == 0, 1.0, 0.0).astype(BF)

    for d in range(count):
        qs[jnp.bitwise_and(me - d, count - 1)] = arrivals[d][...]

    lines = []
    for j in range(count):
        g = gates[pl.ds(k0 + j * kstep, 1), :]
        lines += list(split3((g[:, :1] - g) * LOG2E))
    lines += [jnp.zeros((hd - 3 * count, blk), F32)]
    bias[...] = jnp.concatenate(lines, axis=0).T.astype(BF)
    col = lax.broadcasted_iota(jnp.int32, (blk, hd), 1)

    def shift(qi, ki):
        return (base[q0 + qi * qstep] - base[k0 + ki * kstep]) * LOG2E

    def scores(qi, ki, first=0):
        picked = jnp.where((col >= 3 * ki) & (col < 3 * ki + 3), 1.0, 0.0).astype(BF)
        k = jnp.concatenate([kv_ref[ki, first:, :hd], bias[first:, :]], axis=1)
        return dot(k, jnp.concatenate([qs[qi], picked], axis=1), 1, 1)

    def weighted(ki, p):
        v = [kv_ref[ki, i : i + hd, hd:] for i in range(0, blk, hd)]
        return dot(jnp.concatenate([jnp.concatenate(v, axis=1), count_row], axis=0), p)

    def cross():
        key = lax.broadcasted_iota(jnp.int32, (blk, blk), 0)
        query = lax.broadcasted_iota(jnp.int32, (blk, blk), 1)
        s = jnp.where(key <= query, scores(dq, dk), LOW)
        top = jnp.max(s, axis=0, keepdims=True)
        tops[dq] = top
        acc[dq] = weighted(dk, jnp.exp2(s - top).astype(BF))

    def reference_points():
        for j in range(count):
            kj = tab[2 * steps + 8 + j]
            s = scores(j, kj, blk - 32)
            tops[j] = jnp.max(s, axis=0, keepdims=True) + shift(j, kj)
            acc[j] = jnp.zeros((aug, blk), F32)

    def weigh(t, p_ref):
        qi, ki = tab[t], tab[steps + t]
        sh = jnp.where(t < n, shift(qi, ki), LOW)
        p_ref[...] = jnp.exp2(scores(qi, ki) - (tops[qi] - sh)).astype(BF)

    def add(t, p_ref):
        qi, ki = tab[t], tab[steps + t]
        acc[qi] = acc[qi] + weighted(ki, p_ref[...])

    reference_points()
    cross()

    @pl.when(n > 0)
    def _():
        weigh(0, pa)

    def some_steps(i, c):
        t = UNROLL * i
        for u in range(0, UNROLL, 2):
            weigh(t + u + 1, pb)
            add(t + u, pa)
            weigh(t + u + 2, pa)
            add(t + u + 1, pb)
        return c

    lax.fori_loop(0, (n + UNROLL - 1) // UNROLL, some_steps, 0)

    worst = jnp.zeros((1, blk), F32)
    for j in range(count):
        worst = jnp.maximum(worst, jnp.where(acc[j, hd : hd + 1, :] <= 2.0**100, 0.0, 1.0))

    @pl.when(jnp.max(worst) > 0.0)
    def _():
        def clear(j, c):
            tops[j] = jnp.full((1, blk), LOW, F32)
            acc[j] = jnp.zeros((aug, blk), F32)
            return c

        lax.fori_loop(0, count, clear, 0)
        cross()

        def careful(t, c):
            qi, ki = tab[t], tab[steps + t]
            sh = shift(qi, ki)
            sa[...] = scores(qi, ki)
            before = tops[qi]
            after = jnp.maximum(before, jnp.max(sa[...], axis=0, keepdims=True) + sh)
            tops[qi] = after
            weight = jnp.exp2(sa[...] - (after - sh)).astype(BF)
            acc[qi] = acc[qi] * jnp.exp2(before - after) + weighted(ki, weight)
            return c

        lax.fori_loop(0, n, careful, 0)

    for j in range(count):
        total = acc[j, hd : hd + 1, :]
        some = total > 0.0
        safe = jnp.where(some, total, 1.0)
        over = jnp.where(some, 1.0 / safe, 0.0)
        high, mid, low = split3(jnp.where(some, tops[j] + jnp.log2(safe), LOW))
        o_ref[j, :hd, :] = (acc[j, :hd, :] * over).astype(BF)
        o_ref[j, hd:, :] = jnp.where(
            tail == 0, high, jnp.where(tail == 1, mid, jnp.where(tail == 2, low, 0.0))
        ).astype(BF)


def attend(tab, base, qs, kv, gates):
    count = kv.shape[0]
    blk, hd = qs[0].shape
    aug = hd + 16
    return pl.pallas_call(
        attend_kernel,
        out_shape=jax.ShapeDtypeStruct((count, aug, blk), BF),
        in_specs=[SM, SM] + [VM] * (len(qs) + 2),
        out_specs=VM,
        scratch_shapes=[
            scratch((count, blk, hd), BF),
            scratch((blk, hd), BF),
            scratch((count, aug, blk), F32),
            scratch((count, 1, blk), F32),
            scratch((blk, blk), BF),
            scratch((blk, blk), BF),
            scratch((blk, blk), F32),
        ],
        compiler_params=ROOM,
        name="attend",
    )(tab, base, *qs, kv, gates)


def mix_kernel(where, parts, pool_in, rim, pool_weight, pool_scale, ap_out, wide):
    hd = pool_weight.shape[0]
    rows = pool_in.shape[0]
    count = parts.shape[0]
    lse = []
    for j in range(count):
        t = parts[j, hd : hd + 16, :].astype(F32)
        lse.append(t[0:1] + t[1:2] + t[2:3])
    top = functools.reduce(jnp.maximum, lse)
    total = jnp.zeros_like(top)
    summed = jnp.zeros((hd, rows), F32)
    for j in range(count):
        w = jnp.exp2(lse[j] - top)
        total = total + w
        summed = summed + parts[j, :hd, :].astype(F32) * w
    ap_out[:, :hd] = (summed / total).T.astype(BF)

    first, window = where[1], where[2]
    here = pool_in[...].astype(F32)
    edge = jnp.where(first > 0, rim[...].astype(F32), 0.0)
    wide[:RIM, :] = edge
    wide[RIM:, :] = here
    sums = wide[...]
    span = 1
    chosen = jnp.zeros((rows, hd), F32)
    while span < RIM:
        length = sums.shape[0] - span
        sums = sums[span:, :] + sums[:length, :]
        span *= 2
        at = RIM - span + 1
        chosen = jnp.where(window == span, sums[at : at + rows, :], chosen)
    place = first + lax.broadcasted_iota(jnp.int32, (rows, hd), 0)
    counts = jnp.minimum(window, place + 1).astype(F32)
    departure = (chosen / counts - here).astype(BF)
    ap_out[:, hd:] = (dot(departure, pool_weight[...]) * pool_scale[...]).astype(BF)


def mix(where, parts, pool_in, rim, pool_weight, pool_scale):
    rows, hd = pool_in.shape
    return pl.pallas_call(
        mix_kernel,
        out_shape=placed((rows, 2 * hd), BF),
        in_specs=[SM] + [VM] * 5,
        out_specs=VM,
        scratch_shapes=[scratch((rows + RIM, hd), F32)],
        compiler_params=ROOM,
        name="mix",
    )(where, parts, pool_in, rim, pool_weight, pool_scale)


def out_kernel(where, mine, theirs, wa, wp, wt, out):
    odd = where[0]
    rows = mine.shape[0]
    hd = wa.shape[0]
    a = jnp.concatenate([mine[...], theirs[...]], axis=1)
    for x in range(out.shape[0]):
        wide = out.shape[2]
        at = pl.multiple_of((2 * x + odd) * wide, wide)
        w = jnp.concatenate(
            [wa[:, pl.ds(at, wide)], wp[:, pl.ds(at, wide)], wt[:, x * wide : (x + 1) * wide]], axis=0
        )
        out[x] = dot(a, w).astype(BF)


def out_project(where, mine, theirs, wa, wp, wt, chips):
    rows = mine.shape[0]
    wide = wt.shape[1] // chips
    return pl.pallas_call(
        out_kernel,
        out_shape=placed((chips, rows, wide), BF),
        in_specs=[SM] + [VM] * 5,
        out_specs=VM,
        compiler_params=ROOM,
        name="out_project",
    )(where, mine, theirs, wa, wp, wt)


def square_kernel(parts, mixed_out, sq_out):
    rows, wide = mixed_out.shape
    mixed = functools.reduce(lambda a, b: a + b, [parts[x].astype(F32) for x in range(parts.shape[0])])
    mixed_out[...] = mixed
    sq = mixed * mixed
    lanes = functools.reduce(lambda a, b: a + b, [sq[:, i : i + 128] for i in range(0, wide, 128)])
    for r in range(rows // 128):
        line = jnp.sum(lanes[r * 128 : (r + 1) * 128, :].T, axis=0, keepdims=True)
        for i in range(sq_out.shape[0]):
            sq_out[i, r : r + 1, :] = line


def square(parts):
    chips, rows, wide = parts.shape
    return pl.pallas_call(
        square_kernel,
        out_shape=(
            placed((rows, wide), F32),
            placed((8, rows // 128, 128), F32),
        ),
        in_specs=[VM],
        out_specs=(VM, VM),
        compiler_params=ROOM,
        name="square",
    )(parts)


def finish_kernel(mixed, sq, gain, out, *, width):
    total = functools.reduce(lambda a, b: a + b, [sq[i] for i in range(sq.shape[0])])
    inverse = lax.rsqrt(total / width + EPS)
    for r in range(total.shape[0]):
        each = jnp.broadcast_to(inverse[r : r + 1, :], (128, 128)).T
        for c in range(0, mixed.shape[1], 128):
            at = slice(r * 128, (r + 1) * 128)
            out[at, c : c + 128] = (mixed[at, c : c + 128] * each * gain[:, c : c + 128]).astype(BF)


def finish_rows(mixed, sq, gain, width):
    rows, wide = mixed.shape
    return pl.pallas_call(
        functools.partial(finish_kernel, width=width),
        out_shape=jax.ShapeDtypeStruct((rows, wide), BF),
        in_specs=[VM] * 3,
        out_specs=VM,
        compiler_params=ROOM,
        name="finish",
    )(mixed, sq, gain)


CHIPS = [[0, 2, 4, 6], [1, 3, 5, 7]]
PARTNER = [(i, i ^ 1) for i in range(8)]


def exchange(blocks, axis, groups):
    return near(lax.all_to_all(blocks, axis, 0, 0, axis_index_groups=groups, tiled=True))


def permute(x, axis, route):
    return near(lax.ppermute(x, axis, route))


def body(
    tokens,
    input_gain,
    query_weight,
    key_weight,
    value_weight,
    pool_in_weight,
    log_gates,
    pool_weight,
    pool_scale,
    attention_out,
    pooling_out,
    final_gain,
):
    rows, wide = tokens.shape
    width = query_weight.shape[0]
    hd = pool_weight.shape[1]
    sp = lax.axis_index("sp")
    tp = lax.axis_index("tp")
    odd = tp % 2
    where = jnp.stack([odd, sp * rows, jnp.left_shift(2, tp % 4)]).astype(jnp.int32)

    def for_partner(w):
        return lax.dynamic_index_in_dim(w.reshape(hd, 4, 2, wide), 1 - odd, 2, keepdims=False).reshape(hd, 4 * wide)

    theirs = jnp.concatenate([for_partner(attention_out), for_partner(pooling_out)], axis=0)
    partner_weight = permute(theirs, "tp", PARTNER)

    extended = jnp.concatenate([tokens, jnp.broadcast_to(input_gain, (16, wide))], axis=0)
    own = exchange(jnp.broadcast_to(extended, (4, rows + 16, wide)), "tp", CHIPS)
    other = permute(own, "tp", PARTNER)
    q, kv, pool_in = project(
        where, own, other, query_weight, key_weight, value_weight, pool_in_weight, rows, hd
    )

    sequence = lax.axis_size("sp")
    rim = permute(pool_in[rows - RIM :], "sp", [(i, i + 1) for i in range(sequence - 1)])
    kv = exchange(kv, BOTH, rings(True))
    qs = [near(q)] + [permute(q, BOTH, moved(d)) for d in range(1, SIDE)]

    gates = log_gates.reshape(sequence, rows)
    table = jnp.asarray(work_table())
    tab = lax.dynamic_slice(table, (odd, sp, 0), (1, 1, table.shape[2])).reshape(-1)
    parts = attend(tab, gates[:, 0], qs, kv, gates)
    parts = exchange(parts, BOTH, rings(False))

    ap = mix(where, parts, near(pool_in), rim, pool_weight[0], pool_scale.reshape(1, -1))
    ap_other = permute(ap, "tp", PARTNER)
    shares = out_project(where, near(ap), ap_other, attention_out, pooling_out, partner_weight, 4)
    mixed, sq = square(exchange(shares, "tp", CHIPS))
    sq = near(lax.all_to_all(sq, "tp", 0, 0, tiled=True))
    return finish_rows(near(mixed), sq, final_gain.reshape(1, -1), width)


def solution(mesh):
    return jax.shard_map(
        body,
        mesh=mesh,
        in_specs=(
            P("sp", "tp"),
            P("tp"),
            P(None, "tp"),
            P(None, "tp"),
            P(None, "tp"),
            P(None, "tp"),
            P("tp", None),
            P("tp", None, None),
            P("tp"),
            P("tp", None),
            P("tp", None),
            P("tp"),
        ),
        out_specs=P("sp", "tp"),
        check_vma=False,
    )
```

```python
import functools
import math

import jax
import jax.numpy as jnp
from jax import lax
from jax.experimental import pallas as pl
from jax.experimental.pallas import tpu as pltpu
from jax.sharding import PartitionSpec as P

BF = jnp.bfloat16
F32 = jnp.float32
LOW = -1e30
EPS = 1e-06
LOG2E = math.log2(math.e)
RIM = 16
BOTH = ("sp", "tp")
SIDE = 8
UNROLL = 8

VM = pl.BlockSpec(memory_space=pltpu.VMEM)
SM = pl.BlockSpec(memory_space=pltpu.SMEM)
ROOM = pltpu.CompilerParams(vmem_limit_bytes=56 * 2**20)


def scratch(shape, dtype):
    return pltpu.VMEM(shape, dtype)


def placed(shape, dtype):
    return pltpu.VMEM(shape, dtype)


def near(x):
    return pltpu.with_memory_space_constraint(x, pltpu.VMEM)


def ring(z, y, p, along_y):
    return [((z * SIDE + i) if along_y else (i * SIDE + y)) * 8 + p for i in range(SIDE)]


def rings(for_keys):
    groups = []
    for p in range(8):
        along_y = (p % 2 == 0) == for_keys
        for i in range(SIDE):
            groups.append(ring(i, i, p, along_y))
    return groups


def moved(distance, for_keys=False, y_too=True):
    route = []
    for group in rings(for_keys):
        along_y = (group[0] % 2 == 0) == for_keys
        for i in range(SIDE):
            j = (i + distance) % SIDE
            if (y_too if along_y else (j > i if for_keys else j < i)):
                route.append((group[i], group[j]))
    return route


def passed_on(distance, for_keys):
    return [
        (group[i], group[(i + distance) % SIDE])
        for group in rings(for_keys)
        if (group[0] % 2 == 0) == for_keys
        for i in range(SIDE)
    ]


def split3(x):
    high = x.astype(BF).astype(F32)
    rest = x - high
    mid = rest.astype(BF).astype(F32)
    return high, mid, rest - mid


def dot(a, b, ca=1, cb=0):
    return lax.dot_general(a, b, (((ca,), (cb,)), ((), ())), preferred_element_type=F32)


def spread_kernel(tokens, gain, out):
    rows = tokens.shape[0]
    t = tokens[...]
    g = jnp.broadcast_to(gain[...].astype(F32).reshape(1, -1), (16, tokens.shape[1])).astype(BF)
    for x in range(out.shape[0]):
        out[x, :rows, :] = t
        out[x, rows:, :] = g


def spread(tokens, gain, chips):
    rows, wide = tokens.shape
    return pl.pallas_call(
        spread_kernel,
        out_shape=placed((chips, rows + 16, wide), BF),
        in_specs=[VM] * 2,
        out_specs=VM,
        compiler_params=ROOM,
        name="spread",
    )(tokens, gain)


def products(ref, parity, weights, rows):
    wq, wk, wv, wp = weights
    wide = ref.shape[2]
    squares, qp, kv = 0.0, 0.0, 0.0
    for x in range(ref.shape[0]):
        at = pl.multiple_of((2 * x + parity) * wide, wide)
        t = ref[x, :rows, :].astype(F32)
        gain = ref[x, rows : rows + 1, :].astype(F32)
        sq = t * t
        squares = squares + functools.reduce(lambda a, b: a + b, [sq[:, i : i + 128] for i in range(0, wide, 128)])
        s = (t * gain).astype(BF)
        w1 = jnp.concatenate([wq[pl.ds(at, wide), :], wp[pl.ds(at, wide), :]], axis=1)
        w2 = jnp.concatenate([wk[pl.ds(at, wide), :], wv[pl.ds(at, wide), :]], axis=1)
        qp = qp + dot(s, w1)
        kv = kv + dot(s, w2)
    return squares, qp, kv


def own_kernel(where, own, wq, wk, wv, wp, sq_out, qp_out, kv_out):
    sq_out[...], qp_out[...], kv_out[...] = products(own, where[0], (wq, wk, wv, wp), sq_out.shape[0])


def rest_kernel(where, other, wq, wk, wv, wp, sq_in, qp_in, kv_in, q_out, kv_out, p_out, *, factor):
    rows = q_out.shape[0]
    squares, qp, kv = products(other, 1 - where[0], (wq, wk, wv, wp), rows)
    squares = squares + sq_in[...]
    qp = qp + qp_in[...]
    kv = kv + kv_in[...]
    width = wq.shape[0]
    inverse = lax.rsqrt(jnp.sum(squares, axis=1, keepdims=True) / width + EPS)
    q_out[...] = (qp[:, :128] * (inverse * factor)).astype(BF)
    p_out[...] = (qp[:, 128:] * inverse).astype(BF)
    k = (kv[:, :128] * inverse).astype(BF)
    vt = (kv[:, 128:] * inverse).T.astype(BF)
    kv_out[:, :128] = k
    for r in range(0, rows, 128):
        kv_out[r : r + 128, 128:] = vt[:, r : r + 128]


def project_own(where, own, weights, rows):
    return pl.pallas_call(
        own_kernel,
        out_shape=(placed((rows, 128), F32), placed((rows, 256), F32), placed((rows, 256), F32)),
        in_specs=[SM] + [VM] * 5,
        out_specs=(VM, VM, VM),
        compiler_params=ROOM,
        name="project_own",
    )(where, own, *weights)


def project_rest(where, other, weights, partial, rows, head):
    factor = head ** (-0.5) * LOG2E
    return pl.pallas_call(
        functools.partial(rest_kernel, factor=factor),
        out_shape=(
            placed((rows, head), BF),
            placed((rows, 2 * head), BF),
            placed((rows, head), BF),
        ),
        in_specs=[SM] + [VM] * 8,
        out_specs=(VM, VM, VM),
        compiler_params=ROOM,
        name="project_rest",
    )(where, other, *weights, *[near(t) for t in partial])


def attend_kernel(where, *refs):
    many = SIDE + 1
    q_in, kv_in = refs[:many], refs[many : 2 * many]
    gates, o_ref, qs, kv_ref, bias, acc, tops, bases, pa, pb, sa = refs[2 * many :]
    count = SIDE
    blk, hd = q_in[0].shape
    aug = acc.shape[1]
    odd, z, y = where[0], where[3] >> 3, where[3] & 7
    even = odd == 0

    def pick(a, b):
        return jnp.where(even, a, b)

    dq, dk = pick(z, y), pick(y, z)
    me, key_me = dq, dk
    q0, qstep, k0, kstep = pick(y, 8 * z), pick(8, 1), pick(8 * z, y), pick(1, 8)
    n = pick(8 * (7 - z) + y, 8 * z + 7 - y)

    def pair(t):
        t = jnp.minimum(t, n - 1)
        later = t - y
        past = t - 8 * z
        even_q = jnp.where(later < 0, z, z + 1 + (later >> 3))
        even_k = jnp.where(later < 0, t, later & 7)
        odd_q = jnp.where(past < 0, t & 7, y + 1 + past)
        odd_k = jnp.where(past < 0, t >> 3, z)
        return pick(even_q, odd_q), pick(even_k, odd_k)

    def nearest(qi):
        even_k = jnp.where(qi > z, 7, jnp.where(qi == z, y - 1, 0))
        odd_k = jnp.where(qi > y, z, z - 1)
        return jnp.maximum(pick(even_k, odd_k), 0)

    tail = lax.broadcasted_iota(jnp.int32, (aug - hd, blk), 0)
    count_row = jnp.where(tail == 0, 1.0, 0.0).astype(BF)
    tail8 = tail[:8]

    for d in range(count):
        if d != count // 2:
            qs[jnp.bitwise_and(me - d, count - 1)] = q_in[d][...]
            kv_ref[jnp.bitwise_and(key_me - d, count - 1)] = kv_in[d][...]
    far_q = jnp.bitwise_and(me - count // 2, count - 1)
    far_k = jnp.bitwise_and(key_me - count // 2, count - 1)

    @pl.when(odd == 0)
    def _():
        qs[far_q] = q_in[count // 2][...]
        kv_ref[far_k] = kv_in[count][...]

    @pl.when(odd == 1)
    def _():
        qs[far_q] = q_in[count][...]
        kv_ref[far_k] = kv_in[count // 2][...]

    lines = []
    for j in range(count):
        g = gates[:, pl.ds(pl.multiple_of((k0 + j * kstep) * blk, blk), blk)]
        first = jnp.broadcast_to(g[:, :1], (1, blk))
        bases[count + j] = first
        lines += list(split3((first - g) * LOG2E))
        g = gates[:, pl.ds(pl.multiple_of((q0 + j * qstep) * blk, blk), blk)]
        bases[j] = jnp.broadcast_to(g[:, :1], (1, blk))
    lines += [jnp.zeros((hd - 3 * count, blk), F32)]
    bias[...] = jnp.concatenate(lines, axis=0).T.astype(BF)
    col = lax.broadcasted_iota(jnp.int32, (blk, hd), 1)

    def shift(qi, ki):
        return (bases[qi] - bases[count + ki]) * LOG2E

    def scores(qi, ki, first=0):
        picked = jnp.where((col >= 3 * ki) & (col < 3 * ki + 3), 1.0, 0.0).astype(BF)
        k = jnp.concatenate([kv_ref[ki, first:, :hd], bias[first:, :]], axis=1)
        return dot(k, jnp.concatenate([qs[qi], picked], axis=1), 1, 1)

    def weighted(ki, p):
        v = [kv_ref[ki, i : i + hd, hd:] for i in range(0, blk, hd)]
        return dot(jnp.concatenate([jnp.concatenate(v, axis=1), count_row], axis=0), p)

    def cross():
        key = lax.broadcasted_iota(jnp.int32, (blk, blk), 0)
        query = lax.broadcasted_iota(jnp.int32, (blk, blk), 1)
        s = jnp.where(key <= query, scores(dq, dk), LOW)
        top = jnp.max(s, axis=0, keepdims=True)
        tops[dq] = top
        acc[dq] = weighted(dk, jnp.exp2(s - top).astype(BF))

    def reference_points():
        for j in range(count):
            kj = nearest(j)
            s = scores(j, kj, blk - 32)
            tops[j] = jnp.max(s, axis=0, keepdims=True) + shift(j, kj)
            acc[j] = jnp.zeros((aug, blk), F32)

    def weigh(t, p_ref):
        qi, ki = pair(t)
        sh = jnp.where(t < n, shift(qi, ki), LOW)
        p_ref[...] = jnp.exp2(scores(qi, ki) - (tops[qi] - sh)).astype(BF)

    def add(t, p_ref):
        qi, ki = pair(t)
        acc[qi] = acc[qi] + weighted(ki, p_ref[...])

    reference_points()
    cross()

    @pl.when(n > 0)
    def _():
        weigh(0, pa)

    def some_steps(i, c):
        t = UNROLL * i
        for u in range(0, UNROLL, 2):
            weigh(t + u + 1, pb)
            add(t + u, pa)
            weigh(t + u + 2, pa)
            add(t + u + 1, pb)
        return c

    lax.fori_loop(0, (n + UNROLL - 1) // UNROLL, some_steps, 0)

    worst = jnp.zeros((1, blk), F32)
    for j in range(count):
        worst = jnp.maximum(worst, jnp.where(acc[j, hd : hd + 1, :] <= 2.0**100, 0.0, 1.0))

    @pl.when(jnp.max(worst) > 0.0)
    def _():
        def clear(j, c):
            tops[j] = jnp.full((1, blk), LOW, F32)
            acc[j] = jnp.zeros((aug, blk), F32)
            return c

        lax.fori_loop(0, count, clear, 0)
        cross()

        def careful(t, c):
            qi, ki = pair(t)
            sh = shift(qi, ki)
            sa[...] = scores(qi, ki)
            before = tops[qi]
            after = jnp.maximum(before, jnp.max(sa[...], axis=0, keepdims=True) + sh)
            tops[qi] = after
            weight = jnp.exp2(sa[...] - (after - sh)).astype(BF)
            acc[qi] = acc[qi] * jnp.exp2(before - after) + weighted(ki, weight)
            return c

        lax.fori_loop(0, n, careful, 0)

    for j in range(count):
        total = acc[j, hd : hd + 1, :]
        some = total > 0.0
        safe = jnp.where(some, total, 1.0)
        over = jnp.where(some, 1.0 / safe, 0.0)
        high, mid, low = split3(jnp.where(some, tops[j] + jnp.log2(safe), LOW))
        o_ref[j, :hd, :] = (acc[j, :hd, :] * over).astype(BF)
        o_ref[j, hd:, :] = jnp.where(
            tail8 == 0, high, jnp.where(tail8 == 1, mid, jnp.where(tail8 == 2, low, 0.0))
        ).astype(BF)


def attend(where, qs, kvs, gates):
    count = SIDE
    blk, hd = qs[0].shape
    aug = hd + 16
    return pl.pallas_call(
        attend_kernel,
        out_shape=jax.ShapeDtypeStruct((count, hd + 8, blk), BF),
        in_specs=[SM] + [VM] * (2 * SIDE + 3),
        out_specs=VM,
        scratch_shapes=[
            scratch((count, blk, hd), BF),
            scratch((count, blk, 2 * hd), BF),
            scratch((blk, hd), BF),
            scratch((count, aug, blk), F32),
            scratch((count, 1, blk), F32),
            scratch((2 * count, 1, blk), F32),
            scratch((blk, blk), BF),
            scratch((blk, blk), BF),
            scratch((blk, blk), F32),
        ],
        compiler_params=ROOM,
        name="attend",
    )(where, *qs, *kvs, gates)


def mix_kernel(where, parts, pool_in, rim, pool_weight, pool_scale, ap_out, wide):
    hd = pool_weight.shape[0]
    rows = pool_in.shape[0]
    count = parts.shape[0]
    lse = []
    for j in range(count):
        t = parts[j, hd : hd + 8, :].astype(F32)
        lse.append(t[0:1] + t[1:2] + t[2:3])
    top = functools.reduce(jnp.maximum, lse)
    total = jnp.zeros_like(top)
    summed = jnp.zeros((hd, rows), F32)
    for j in range(count):
        w = jnp.exp2(lse[j] - top)
        total = total + w
        summed = summed + parts[j, :hd, :].astype(F32) * w
    ap_out[:, :hd] = (summed / total).T.astype(BF)

    first, window = where[1], where[2]
    here = pool_in[...].astype(F32)
    edge = jnp.where(first > 0, rim[...].astype(F32), 0.0)
    wide[:RIM, :] = edge
    wide[RIM:, :] = here
    sums = wide[...]
    span = 1
    chosen = jnp.zeros((rows, hd), F32)
    while span < RIM:
        length = sums.shape[0] - span
        sums = sums[span:, :] + sums[:length, :]
        span *= 2
        at = RIM - span + 1
        chosen = jnp.where(window == span, sums[at : at + rows, :], chosen)
    place = first + lax.broadcasted_iota(jnp.int32, (rows, hd), 0)
    counts = jnp.minimum(window, place + 1).astype(F32)
    departure = (chosen / counts - here).astype(BF)
    ap_out[:, hd:] = (dot(departure, pool_weight[...]) * pool_scale[...]).astype(BF)


def mix(where, parts, pool_in, rim, pool_weight, pool_scale):
    rows, hd = pool_in.shape
    return pl.pallas_call(
        mix_kernel,
        out_shape=placed((rows, 2 * hd), BF),
        in_specs=[SM] + [VM] * 5,
        out_specs=VM,
        scratch_shapes=[scratch((rows + RIM, hd), F32)],
        compiler_params=ROOM,
        name="mix",
    )(where, parts, pool_in, rim, pool_weight, pool_scale)


def out_kernel(where, mine, theirs, wa, wp, wt, out):
    odd = where[0]
    rows = mine.shape[0]
    hd = wa.shape[0]
    a = jnp.concatenate([mine[...], theirs[...]], axis=1)
    for x in range(out.shape[0]):
        wide = out.shape[2]
        at = pl.multiple_of((2 * x + odd) * wide, wide)
        w = jnp.concatenate(
            [wa[:, pl.ds(at, wide)], wp[:, pl.ds(at, wide)], wt[:, x * wide : (x + 1) * wide]], axis=0
        )
        out[x] = dot(a, w).astype(BF)


def out_project(where, mine, theirs, wa, wp, wt, chips):
    rows = mine.shape[0]
    wide = wt.shape[1] // chips
    return pl.pallas_call(
        out_kernel,
        out_shape=placed((chips, rows, wide), BF),
        in_specs=[SM] + [VM] * 5,
        out_specs=VM,
        compiler_params=ROOM,
        name="out_project",
    )(where, mine, theirs, wa, wp, wt)


def square_kernel(parts, mixed_out, sq_out):
    rows, wide = mixed_out.shape
    mixed = functools.reduce(lambda a, b: a + b, [parts[x].astype(F32) for x in range(parts.shape[0])])
    mixed_out[...] = mixed
    sq = mixed * mixed
    lanes = functools.reduce(lambda a, b: a + b, [sq[:, i : i + 128] for i in range(0, wide, 128)])
    for r in range(rows // 128):
        line = jnp.sum(lanes[r * 128 : (r + 1) * 128, :].T, axis=0, keepdims=True)
        for i in range(sq_out.shape[0]):
            sq_out[i, r : r + 1, :] = line


def square(parts):
    chips, rows, wide = parts.shape
    return pl.pallas_call(
        square_kernel,
        out_shape=(
            placed((rows, wide), F32),
            placed((8, rows // 128, 128), F32),
        ),
        in_specs=[VM],
        out_specs=(VM, VM),
        compiler_params=ROOM,
        name="square",
    )(parts)


def finish_kernel(mixed, sq, gain, out, *, width):
    total = functools.reduce(lambda a, b: a + b, [sq[i] for i in range(sq.shape[0])])
    inverse = lax.rsqrt(total / width + EPS)
    for r in range(total.shape[0]):
        each = jnp.broadcast_to(inverse[r : r + 1, :], (128, 128)).T
        for c in range(0, mixed.shape[1], 128):
            at = slice(r * 128, (r + 1) * 128)
            out[at, c : c + 128] = (mixed[at, c : c + 128] * each * gain[:, c : c + 128]).astype(BF)


def finish_rows(mixed, sq, gain, width):
    rows, wide = mixed.shape
    return pl.pallas_call(
        functools.partial(finish_kernel, width=width),
        out_shape=jax.ShapeDtypeStruct((rows, wide), BF),
        in_specs=[VM] * 3,
        out_specs=VM,
        compiler_params=ROOM,
        name="finish",
    )(mixed, sq, gain)


CHIPS = [[0, 2, 4, 6], [1, 3, 5, 7]]
PARTNER = [(i, i ^ 1) for i in range(8)]


def exchange(blocks, axis, groups):
    return near(lax.all_to_all(blocks, axis, 0, 0, axis_index_groups=groups, tiled=True))


def permute(x, axis, route):
    return near(lax.ppermute(x, axis, route))


def body(
    tokens,
    input_gain,
    query_weight,
    key_weight,
    value_weight,
    pool_in_weight,
    log_gates,
    pool_weight,
    pool_scale,
    attention_out,
    pooling_out,
    final_gain,
):
    rows, wide = tokens.shape
    width = query_weight.shape[0]
    hd = pool_weight.shape[1]
    sp = lax.axis_index("sp")
    tp = lax.axis_index("tp")
    odd = tp % 2
    where = jnp.stack([odd, sp * rows, jnp.left_shift(2, tp % 4), sp]).astype(jnp.int32)

    def for_partner(w):
        return lax.dynamic_index_in_dim(w.reshape(hd, 4, 2, wide), 1 - odd, 2, keepdims=False).reshape(hd, 4 * wide)

    theirs = jnp.concatenate([for_partner(attention_out), for_partner(pooling_out)], axis=0)
    partner_weight = permute(theirs, "tp", PARTNER)

    weights = [near(w) for w in (query_weight, key_weight, value_weight, pool_in_weight)]
    own = exchange(spread(tokens, input_gain, 4), "tp", CHIPS)
    other = permute(own, "tp", PARTNER)
    partial = project_own(where, own, weights, rows)
    q, kv, pool_in = project_rest(where, other, weights, partial, rows, hd)

    sequence = lax.axis_size("sp")
    rim = permute(pool_in[rows - RIM :], "sp", [(i, i + 1) for i in range(sequence - 1)])
    qs, kvs = [near(q)], [near(kv)]
    half = SIDE // 2
    for d in range(1, SIDE):
        kvs.append(permute(kv, BOTH, moved(d, True, d != half)))
        qs.append(permute(q, BOTH, moved(d, False, d != half)))
    kvs.append(permute(kvs[half + 1], BOTH, passed_on(-1, True)))
    qs.append(permute(qs[half - 1], BOTH, passed_on(1, False)))

    parts = attend(where, qs, kvs, near(log_gates))
    parts = exchange(parts, BOTH, rings(False))

    ap = mix(where, parts, near(pool_in), rim, pool_weight[0], pool_scale.reshape(1, -1))
    ap_other = permute(ap, "tp", PARTNER)
    shares = out_project(where, near(ap), ap_other, near(attention_out), near(pooling_out), partner_weight, 4)
    mixed, sq = square(exchange(shares, "tp", CHIPS))
    sq = near(lax.all_to_all(sq, "tp", 0, 0, tiled=True))
    return finish_rows(near(mixed), sq, final_gain.reshape(1, -1), width)


def solution(mesh):
    return jax.shard_map(
        body,
        mesh=mesh,
        in_specs=(
            P("sp", "tp"),
            P("tp"),
            P(None, "tp"),
            P(None, "tp"),
            P(None, "tp"),
            P(None, "tp"),
            P("tp", None),
            P("tp", None, None),
            P("tp"),
            P("tp", None),
            P("tp", None),
            P("tp"),
        ),
        out_specs=P("sp", "tp"),
        check_vma=False,
    )
```
